32 devices in a mesh: ep: 16 (over z, x, core), tp: 2 (over y).
Axes of the slice: x: 2, y: 2, z: 4, core: 2. Of those that a mesh axis runs over, the one named last changes fastest.
Arguments:
- tokens: bfloat16 [208, 1024], P('ep'), may hold values from -60 to 60
- attn_gain: float32 [1024], replicated, may hold values from 0.1 to 1.9
- query_weight: bfloat16 [1024, 512], P(None, 'tp'), may hold values from -0.1875 to 0.1875
- key_weight: bfloat16 [1024, 256], P(None, 'tp'), may hold values from -0.1875 to 0.1875
- value_weight: bfloat16 [1024, 256], P(None, 'tp'), may hold values from -0.1875 to 0.1875
- forget_weight: bfloat16 [1024, 8], P(None, 'tp'), may hold values from -0.5 to 0.5
- forget_bias: float32 [8], P('tp'), may hold values from -3 to 3
- out_weight: bfloat16 [512, 1024], P('tp'), may hold values from -0.75 to 0.75
- key_cache: bfloat16 [208, 4, 64, 1024], P('ep', 'tp'), may hold values from -300 to 300
- value_cache: bfloat16 [208, 4, 64, 1024], P('ep', 'tp'), may hold values from -12 to 12
- cum_forget: float32 [208, 8, 1024], P('ep', 'tp'), may hold values from -131 to 0, as said below
- lengths: int32 [208], P('ep'), may hold values from 256 to 1024
- ffn_gain: float32 [1024], replicated, may hold values from 0.1 to 1.9
- routes: int32 [208, 2], P('ep'), may hold values from 0 to 3, all different within a row; in each aligned block of 13 rows (0 to 12, 13 to 25, ...) at most 13 rows name the same one
- route_weights: float32 [208, 2], P('ep'), may hold values from 0.2 to 1
- gate_weight: bfloat16 [16, 1024, 512], P('ep', None, 'tp'), may hold values from -0.1875 to 0.1875
- up_weight: bfloat16 [16, 1024, 512], P('ep', None, 'tp'), may hold values from -0.1875 to 0.1875
- down_weight: bfloat16 [16, 512, 1024], P('ep', 'tp'), may hold values from -0.25 to 0.25
Outputs:
- layer_out: bfloat16 [208, 1024], P('ep', 'tp')
The draws below stay inside these ranges and needn't reach their ends.
Inputs may be any that keep to these rules, and one draw needn't show every extreme that they name: `routes`: the experts of a row differ; in each aligned block of 13 rows (the rows of one index of ep) no expert is named by more than 13 rows. `cum_forget`: for each sequence and head the entries do not increase along positions.
All inputs are finite; a program needn't handle non-finite values.
Results may differ from the reference program's by a relative error of at most 0.0085.
Values may be sent and summed in bfloat16 or wider, within the bound.
A program may use at most 64 MiB of HBM per device.

```python
import math
import jax
import jax.numpy as jnp
import numpy as np
from jax import lax

D = 1024
HEADS = 8
KVH = 4
HD = 64
FF = 2048
SLICES = 4
TOP_K = 2
SEQ_DEV = 13
STORED_SPAN = 1024
STREAM_TOTAL = 208
EXPERTS = 4
CAP = 13
N_EP = 16
N_TP = 2


def draw_tokens(key, part):
    base_key, row_key = jax.random.split(key, 2)
    column = jnp.arange(D, dtype=jnp.float32) / (D - 1)
    values = jax.random.normal(base_key, (STREAM_TOTAL, D), jnp.float32)
    values = values * jnp.exp(jnp.log(10.0) * column)[None, :]
    row_scale = jnp.exp(jax.random.uniform(row_key, (STREAM_TOTAL, 1), jnp.float32, jnp.log(0.5), jnp.log(2.0)))
    return jnp.clip(values * row_scale, -60.0, 60.0).astype(jnp.bfloat16)


def draw_key_cache(key, part):
    noise_key = jax.random.fold_in(key, 0)
    shape = (STREAM_TOTAL, KVH, HD, STORED_SPAN)
    base = jax.random.normal(noise_key, shape, jnp.float32)
    return jnp.clip(base, -300.0, 300.0).astype(jnp.bfloat16)


def draw_value_cache(key, part):
    noise_key, level_key = jax.random.split(key, 2)
    blocks = STORED_SPAN // 64
    levels = jax.random.normal(level_key, (STREAM_TOTAL, KVH, HD, blocks, 1), jnp.float32)
    noise = jax.random.normal(noise_key, (STREAM_TOTAL, KVH, HD, blocks, 64), jnp.float32)
    return jnp.clip((noise + levels).reshape(STREAM_TOTAL, KVH, HD, STORED_SPAN), -12.0, 12.0).astype(jnp.bfloat16)


def draw_cum_forget(key, part):
    category_noise_seed, gradual_noise_seed, quick_noise_seed, stream_noise_seed, decoding_noise_seed, spike_noise_seed, layering_noise_seed = jax.random.split(key, 7)
    chance = 0.5
    fast = jax.random.uniform(category_noise_seed, (1, HEADS, 1), jnp.float32) < chance
    slow_rate = jax.random.uniform(gradual_noise_seed, (1, HEADS, 1), jnp.float32, 0.2, 0.6) / STORED_SPAN
    fast_rate = jax.random.uniform(quick_noise_seed, (1, HEADS, 1), jnp.float32, 1.0 / 50.0, 1.0 / 30.0)
    rate = jnp.where(fast, fast_rate, slow_rate)
    factor = jnp.exp(jax.random.uniform(stream_noise_seed, (STREAM_TOTAL, 1, 1), jnp.float32, jnp.log(0.5), jnp.log(2.0)))
    rough = jax.random.uniform(decoding_noise_seed, (STREAM_TOTAL, HEADS, STORED_SPAN), jnp.float32, 0.5, 1.5)
    stored_offsets = jax.random.randint(spike_noise_seed, (STREAM_TOTAL, 1, 2), 0, STORED_SPAN)
    position = lax.broadcasted_iota(jnp.int32, (1, 1, STORED_SPAN, 1), 2)
    hits = jnp.sum((position == stored_offsets[:, :, None, :]).astype(jnp.float32), axis=3)
    depth = jax.random.uniform(layering_noise_seed, (STREAM_TOTAL, HEADS, 1), jnp.float32, 0.22, 0.5)
    steps = -rate * factor * rough - hits * depth
    return jnp.clip(jnp.cumsum(steps, axis=2), -(STORED_SPAN // 8) - 3.0, 0.0)


def touch_ends(array, stream_key, low, largest):
    shape = array.shape
    spot = [jax.random.randint(jax.random.fold_in(stream_key, axis), (), 0, shape[axis]) for axis in range(len(shape))]
    array = array.at[tuple(spot)].set(low)
    longest = shape.index(max(shape))
    spot[longest] = (spot[longest] + 1) % shape[longest]
    return array.at[tuple(spot)].set(largest)


def block_scale(rng, shape, shards, low, top_value):
    loudness = 1.0
    for dim, blocks in shards:
        heights = jax.random.uniform(jax.random.fold_in(jax.random.fold_in(rng, 6), dim), (blocks,), jnp.float32, low / len(shards), top_value / len(shards))
        loudness = loudness * jnp.repeat(jnp.exp(heights), shape[dim] // blocks).reshape((-1,) + (1,) * (len(shape) - 1 - dim))
    return loudness


def assign_block(rng, own, number, rows, number_of, top, limit, slope):
    order = jax.random.permutation(rng, number_of)
    heavy_load, common = portions_of(number_of, rows * top, limit, slope, True), portions_of(number_of, rows * top, limit, slope, False)
    places = jnp.arange(number_of)

    def named(tallies, turn):
        used = int((tallies > 0).sum())
        fixed = max(1, used // 4)
        moved = fixed + (places - fixed + turn * (used - fixed)) % max(1, number_of - fixed)
        return jnp.zeros((number_of,), jnp.int32).at[order[jnp.where(places < fixed, places, moved)]].set(jnp.asarray(tallies, jnp.int32))

    tallies = jnp.where(number % 4 == 0, named(heavy_load, number // 4), named(common, number - number // 4 - 1))
    mixed = jax.random.permutation(jax.random.fold_in(own, 3), number_of)
    donor, receiver = mixed[0:number_of // 2 * 2:2], mixed[1:number_of // 2 * 2:2]
    margin = jnp.minimum(tallies[donor] - 1, limit - tallies[receiver]) // 2
    margin = jnp.where((donor == order[0]) | (receiver == order[0]) | (tallies[receiver] == 0), 0, jnp.maximum(margin, 0))
    moved = jax.random.randint(jax.random.fold_in(own, 4), (number_of // 2,), 0, 1 << 20) % (margin + 1)
    tallies = tallies.at[donor].add(-moved).at[receiver].add(moved)
    members = jnp.searchsorted(jnp.cumsum(tallies), jnp.arange(rows * top), side="right").astype(jnp.int32)
    table = members.reshape(top, rows).T
    table = table[jax.random.permutation(jax.random.fold_in(own, 1), rows)]
    turn = jax.random.randint(jax.random.fold_in(own, 2), (rows, 1), 0, top)
    return jnp.take_along_axis(table, (jnp.arange(top)[None, :] + turn) % top, axis=1)


def portions_of(amount, total, limit, slope, full):
    weights = [(1 << 20) // math.isqrt(standing ** slope) + 1 for standing in range(1, amount + 1)]
    largest = limit if full else min(limit, max(-(-total // amount), total * weights[0] // sum(weights)))
    least = 1 if total - largest >= amount - 1 else 0
    holding, surplus = [largest] + [least] * (amount - 1), total - largest - least * (amount - 1)
    while surplus > 0:
        movable = [i for i in range(1, amount) if holding[i] < largest] or [i for i in range(1, amount) if holding[i] < limit]
        pool, budget = sum([weights[i] for i in movable]), surplus
        for i in movable:
            addition = min(limit - holding[i], max(1, budget * weights[i] // pool), surplus)
            holding[i] = holding[i] + addition
            surplus = surplus - addition
    return np.array(holding)


def scatter_about(stream_key, dims, spread, reach, shards=(), kind=jnp.bfloat16):
    array = spread * jax.random.normal(stream_key, dims, jnp.float32)
    if shards:
        array = array * block_scale(stream_key, dims, shards, -0.22, 0.18)
    return jnp.clip(array, -reach, reach).astype(kind)


def setup_inputs(seed: int = 0) -> dict:
    streams_of = jax.random.split(jax.random.key(seed), 19)
    tokens = draw_tokens(jax.random.fold_in(streams_of[18], 71), 0)
    attn_gain = jnp.clip(1.0 + 0.18 * jax.random.normal(streams_of[1], (D,), jnp.float32), 0.1, 1.9)
    query_weight = scatter_about(streams_of[2], (D, HEADS * HD), D ** -0.5, 0.1875, ((1, 2),))
    key_weight = scatter_about(streams_of[3], (D, KVH * HD), D ** -0.5, 0.1875, ((1, 2),))
    value_weight = scatter_about(streams_of[4], (D, KVH * HD), D ** -0.5, 0.1875, ((1, 2),))
    forget_weight = scatter_about(streams_of[5], (D, HEADS), (D // 9) ** -0.5, 0.5, ((1, 2),))
    forget_bias = jnp.clip(jax.random.uniform(streams_of[6], (HEADS,), jnp.float32, -3.0, 3.0) * block_scale(streams_of[6], (HEADS,), ((0, 2),), -0.4, 0.0), -3.0, 3.0)
    out_weight = scatter_about(streams_of[7], (HEADS * HD, D), (HEADS * HD // 8) ** -0.5, 0.75, ((0, 2),))
    key_cache = draw_key_cache(jax.random.fold_in(streams_of[18], 71), 0)
    value_cache = draw_value_cache(jax.random.fold_in(streams_of[18], 71), 0)
    cum_forget = draw_cum_forget(jax.random.fold_in(streams_of[18], 71), 0)
    lengths = touch_ends(jax.random.randint(streams_of[11], (STREAM_TOTAL,), STORED_SPAN // 4, STORED_SPAN + 1), jax.random.fold_in(streams_of[11], 1), STORED_SPAN // 4, STORED_SPAN).astype(jnp.int32)
    ffn_gain = jnp.clip(1.0 + 0.18 * jax.random.normal(streams_of[12], (D,), jnp.float32), 0.1, 1.9)
    routes_keys = jax.random.split(jax.random.fold_in(streams_of[13], 1), STREAM_TOTAL // SEQ_DEV)
    routes_turns = jax.random.permutation(jax.random.fold_in(streams_of[13], 3), STREAM_TOTAL // SEQ_DEV)
    routes = jax.vmap(lambda own, number: assign_block(jax.random.fold_in(streams_of[13], 2), own, number, SEQ_DEV, EXPERTS, TOP_K, CAP, 1))(routes_keys, routes_turns).reshape((STREAM_TOTAL, TOP_K))
    route_weights = jnp.clip(0.2 + 0.8 * jax.random.uniform(streams_of[14], (STREAM_TOTAL, TOP_K), jnp.float32) ** block_scale(streams_of[14], (STREAM_TOTAL, TOP_K), ((0, 16),), -0.2, 0.2), 0.2, 1.0)
    gate_weight = scatter_about(streams_of[15], (EXPERTS * SLICES, D, FF // SLICES), D ** -0.5, 0.1875, ((0, 16), (2, 2)))
    up_weight = scatter_about(streams_of[16], (EXPERTS * SLICES, D, FF // SLICES), D ** -0.5, 0.1875, ((0, 16), (2, 2)))
    down_weight = scatter_about(streams_of[17], (EXPERTS * SLICES, FF // SLICES, D), (FF // 4) ** -0.5, 0.25, ((0, 16), (1, 2)))
    return {"tokens": tokens, "attn_gain": attn_gain, "query_weight": query_weight, "key_weight": key_weight, "value_weight": value_weight, "forget_weight": forget_weight, "forget_bias": forget_bias, "out_weight": out_weight, "key_cache": key_cache, "value_cache": value_cache, "cum_forget": cum_forget, "lengths": lengths, "ffn_gain": ffn_gain, "routes": routes, "route_weights": route_weights, "gate_weight": gate_weight, "up_weight": up_weight, "down_weight": down_weight}


EPSILON = 1e-06

def round_trip(values):
    return lax.optimization_barrier(values.astype(jnp.bfloat16)).astype(jnp.float32)

def normalize(values, gain):
    return values * lax.rsqrt(lax.optimization_barrier(jnp.mean(values * values, axis=-1, keepdims=True)) + EPSILON) * gain

def block_slots(group_routes):
    assigned = group_routes.reshape(-1).astype(jnp.int32)
    member = (assigned[:, None] == jnp.arange(EXPERTS, dtype=jnp.int32)[None, :]).astype(jnp.int32)
    earlier = (jnp.cumsum(member, axis=0) - member).astype(jnp.int32)
    return (assigned * CAP + lax.optimization_barrier(jnp.sum(earlier * member, axis=1))).astype(jnp.int32)

def reference(tokens, attn_gain, query_weight, key_weight, value_weight, forget_weight, forget_bias, out_weight, key_cache, value_cache, cum_forget, lengths, ffn_gain, routes, route_weights, gate_weight, up_weight, down_weight):
    group = HEADS // KVH
    score_scale = HD ** (-0.5)
    token_f = tokens.astype(jnp.float32)
    normed = normalize(token_f, attn_gain).astype(jnp.bfloat16)

    def attend(pack):
        normed_rows, keys, values, cumul, lens = pack
        count = normed_rows.shape[0]
        query_rows = jnp.dot(normed_rows, query_weight, preferred_element_type=jnp.float32).astype(jnp.bfloat16)
        query_rows = query_rows.reshape(count, KVH, group, HD).astype(jnp.float32)
        fresh_keys = jnp.dot(normed_rows, key_weight, preferred_element_type=jnp.float32).astype(jnp.bfloat16)
        fresh_keys = fresh_keys.reshape(count, KVH, HD).astype(jnp.float32)
        new_values = jnp.dot(normed_rows, value_weight, preferred_element_type=jnp.float32).astype(jnp.bfloat16)
        new_values = new_values.reshape(count, KVH, HD).astype(jnp.float32)
        log_forget = jax.nn.log_sigmoid(jnp.dot(normed_rows, forget_weight, preferred_element_type=jnp.float32) + forget_bias)
        log_forget = log_forget.reshape(count, KVH, group)
        scores = jnp.einsum('bkgd,bkdl->bkgl', query_rows, keys.astype(jnp.float32)) * score_scale
        cumul = cumul.reshape(count, KVH, group, STORED_SPAN)
        last_index = jnp.broadcast_to((lens - 1).astype(jnp.int32)[:, None, None, None], (count, KVH, group, 1))
        last = jnp.take_along_axis(cumul, last_index, axis=3)
        positions = jnp.arange(STORED_SPAN, dtype=jnp.int32)[None, None, None, :]
        valid = positions < lens[:, None, None, None]
        scores = jnp.where(valid, scores + (last - cumul) + log_forget[..., None], -jnp.inf)
        self_score = jnp.einsum('qvml,qvl->qvm', query_rows, fresh_keys) * score_scale
        top = jnp.maximum(lax.optimization_barrier(jnp.max(scores, axis=3)), self_score)
        expo = jnp.exp(scores - top[..., None])
        own_exp = jnp.exp(self_score - top)
        total = lax.optimization_barrier(jnp.sum(expo, axis=3)) + own_exp
        weights = round_trip(expo / total[..., None])
        own_weight = round_trip(own_exp / total)
        mixed_heads = jnp.einsum('bkgl,bkdl->bkgd', weights, values.astype(jnp.float32))
        mixed_heads = mixed_heads + own_weight[..., None] * new_values[:, :, None, :]
        heads_out = round_trip(mixed_heads).reshape(count, N_TP, HEADS * HD // N_TP)
        blocks = out_weight.reshape(N_TP, HEADS * HD // N_TP, D).astype(jnp.float32)
        partial_value = jnp.einsum('bnc,ncd->nbd', heads_out, blocks)
        return lax.optimization_barrier(jnp.sum(round_trip(partial_value), axis=0))
    mixed = lax.map(attend, (normed.reshape(N_EP, SEQ_DEV, D), key_cache.reshape(N_EP, SEQ_DEV, KVH, HD, STORED_SPAN), value_cache.reshape(N_EP, SEQ_DEV, KVH, HD, STORED_SPAN), cum_forget.reshape(N_EP, SEQ_DEV, HEADS, STORED_SPAN), lengths.reshape(N_EP, SEQ_DEV))).reshape(STREAM_TOTAL, D)
    residual = round_trip(token_f + mixed)
    ffn_in = normalize(residual, ffn_gain).astype(jnp.bfloat16)
    slots = jax.vmap(block_slots)(routes.reshape(N_EP, SEQ_DEV, TOP_K))
    slot_expert = (slots // CAP).astype(jnp.int32)
    slot_index = (slots % CAP).astype(jnp.int32)
    spread_rows = jnp.repeat(ffn_in.reshape(N_EP, SEQ_DEV, D), TOP_K, axis=1).astype(jnp.float32)
    flat_weights = route_weights.reshape(N_EP, SEQ_DEV * TOP_K)
    units = FF // SLICES
    part_units = units // N_TP
    capacity_iota = jnp.arange(CAP, dtype=jnp.int32)

    def per_expert(routed, pack):
        expert, gates, ups, downs = pack
        chosen = slot_expert == expert
        place = (chosen[:, None, :] & (slot_index[:, None, :] == capacity_iota[None, :, None])).astype(jnp.float32)
        expert_rows = jnp.einsum('gca,gad->gcd', place, spread_rows, precision=lax.Precision.HIGHEST)
        expert_rows = expert_rows.astype(jnp.bfloat16).reshape(N_EP * CAP, D)

        def one_slice(total, weights):
            gate_w, up_w, down_w = weights
            gate = jnp.dot(expert_rows, gate_w, preferred_element_type=jnp.float32)
            up = jnp.dot(expert_rows, up_w, preferred_element_type=jnp.float32)
            hidden = round_trip(jax.nn.silu(gate) * up).reshape(N_EP * CAP, N_TP, part_units)
            parts = jnp.einsum('rnu,nud->nrd', hidden, down_w.reshape(N_TP, part_units, D).astype(jnp.float32))
            return (total + round_trip(lax.optimization_barrier(jnp.sum(round_trip(parts), axis=0))), None)
        served, _ = lax.scan(one_slice, jnp.zeros((N_EP * CAP, D), jnp.float32), (gates, ups, downs))
        picked = jnp.einsum('gca,gcd->gad', place, served.reshape(N_EP, CAP, D), precision=lax.Precision.HIGHEST)
        share = (flat_weights * chosen.astype(jnp.float32))[..., None] * picked
        return (routed + lax.optimization_barrier(jnp.sum(share.reshape(STREAM_TOTAL, TOP_K, D), axis=1)), None)
    routed, _ = lax.scan(per_expert, jnp.zeros((STREAM_TOTAL, D), jnp.float32), (jnp.arange(EXPERTS, dtype=jnp.int32), gate_weight.reshape(EXPERTS, SLICES, D, units), up_weight.reshape(EXPERTS, SLICES, D, units), down_weight.reshape(EXPERTS, SLICES, units, D)))
    return (residual + routed).astype(jnp.bfloat16)
```

```python
import functools

import jax
import jax.numpy as jnp
from jax import lax
from jax.experimental import pallas as pl
from jax.experimental.pallas import tpu as pltpu
from jax.sharding import PartitionSpec as P

HEADS = 8
KVH = 4
HD = 64
SLICES = 4
EPSILON = 1e-06
GROUP_SEQS = 4
MESH = pl.DeviceIdType.MESH
F32 = jnp.float32
BF16 = jnp.bfloat16


def inverse_rms(values):
    return lax.rsqrt(jnp.sum(values * values, axis=-1, keepdims=True) / values.shape[-1] + EPSILON)


def dot(a, b):
    return jnp.dot(a, b, preferred_element_type=F32)


def dot_nt(a, b):
    return lax.dot_general(a, b, (((1,), (1,)), ((), ())), preferred_element_type=F32)


def attention_kernel(
    tokens_ref,
    gain_ref,
    bias_ref,
    lengths_ref,
    wq_hbm,
    wk_hbm,
    wv_hbm,
    wf_ref,
    wo_hbm,
    keys_hbm,
    values_hbm,
    cum_hbm,
    part_ref,
    wq,
    wk,
    wv,
    wo,
    keys,
    values,
    cum,
    q_rows,
    own_rows,
    out_rows,
    w_sem,
    k_sem,
    v_sem,
    c_sem,
):
    rows = tokens_ref.shape[0]
    kv_local, hd, span = keys.shape[1:]
    heads = cum.shape[1]
    group = heads // kv_local
    lanes = kv_local * hd
    scale = hd ** (-0.5)
    w_copies = [
        pltpu.make_async_copy(src, dst, w_sem.at[i])
        for i, (src, dst) in enumerate(((wq_hbm, wq), (wk_hbm, wk), (wv_hbm, wv), (wo_hbm, wo)))
    ]
    for copy in w_copies[:3]:
        copy.start()
    copies = []
    for b in range(rows):
        trio = (
            pltpu.make_async_copy(keys_hbm.at[b], keys.at[b], k_sem.at[b]),
            pltpu.make_async_copy(cum_hbm.at[b], cum.at[b], c_sem.at[b]),
            pltpu.make_async_copy(values_hbm.at[b], values.at[b], v_sem.at[b]),
        )
        for copy in trio:
            copy.start()
        copies.append(trio)
    w_copies[3].start()

    token_f = tokens_ref[...].astype(F32)
    normed = (token_f * inverse_rms(token_f) * gain_ref[...]).astype(BF16)
    head_id = lax.broadcasted_iota(jnp.int32, (heads, 1), 0)
    bias = jnp.zeros((heads, 1), F32)
    for h in range(heads):
        bias = jnp.where(head_id == h, bias_ref[h], bias)
    log_forget = jax.nn.log_sigmoid(dot_nt(wf_ref[...], normed) + bias)
    for copy in w_copies[:3]:
        copy.wait()
    queries = dot(normed, wq[...]).astype(BF16).astype(F32)
    new_keys = dot(normed, wk[...]).astype(BF16).astype(F32)
    new_values = dot(normed, wv[...]).astype(BF16).astype(F32)
    lane_kv = lax.broadcasted_iota(jnp.int32, (rows, lanes), 1) // hd
    q_rows[...] = jnp.zeros_like(q_rows)
    own_rows[...] = jnp.zeros_like(own_rows)
    for h in range(heads):
        kv = h // group
        base = (h * hd) // lanes * lanes
        segment = queries[:, base : base + lanes]
        shift = (kv * hd - (h * hd - base)) % lanes
        if shift:
            segment = pltpu.roll(segment, shift, 1)
        segment = jnp.where(lane_kv == kv, segment, 0.0)
        q_rows[pl.ds(h, rows, stride=8), :] = segment
        own_rows[pl.ds(h, rows, stride=8), :] = segment * new_keys

    position = lax.broadcasted_iota(jnp.int32, (heads, span), 1)
    for first in range(0, rows, GROUP_SEQS):
        members = range(first, min(first + GROUP_SEQS, rows))
        for b in members:
            for copy in copies[b]:
                copy.wait()
        scores = [
            dot(q_rows[b * 8 : b * 8 + 8, :].astype(BF16), keys[b].reshape(lanes, span))[:heads]
            for b in members
        ]
        weights, own = [], []
        for b, score in zip(members, scores):
            cumul = cum[b]
            length = lengths_ref[b]
            last = jnp.sum(jnp.where(position == length - 1, cumul, 0.0), axis=1, keepdims=True)
            score = score * scale + (last - cumul) + log_forget[:, b : b + 1]
            score = jnp.where(position < length, score, -jnp.inf)
            self_score = (
                jnp.sum(own_rows[b * 8 : b * 8 + 8, :], axis=1, keepdims=True)[:heads] * scale
            )
            top = jnp.maximum(jnp.max(score, axis=1, keepdims=True), self_score)
            expo = jnp.exp(score - top)
            own_exp = jnp.exp(self_score - top)
            inverse = 1.0 / (jnp.sum(expo, axis=1, keepdims=True) + own_exp)
            weights.append((expo * inverse).astype(BF16))
            own.append((own_exp * inverse).astype(BF16).astype(F32))
        for b, weight, own_weight in zip(members, weights, own):
            mixed = dot_nt(weight, values[b].reshape(lanes, span))
            out_rows[b * 8 : b * 8 + heads, :] = mixed + own_weight * new_values[b : b + 1, :]

    blocks = []
    for h in range(heads):
        kv = h // group
        base = (h * hd) // lanes * lanes
        segment = out_rows[pl.ds(h, rows, stride=8), :]
        segment = jnp.where(lane_kv == kv, segment, 0.0)
        shift = (h * hd - base - kv * hd) % lanes
        if shift:
            segment = pltpu.roll(segment, shift, 1)
        if base // lanes == len(blocks):
            blocks.append(segment)
        else:
            blocks[-1] = blocks[-1] + segment
    w_copies[3].wait()
    total = None
    for i, block in enumerate(blocks):
        term = dot(block.astype(BF16), wo[i * lanes : (i + 1) * lanes, :])
        total = term if total is None else total + term
    part_ref[...] = jnp.zeros_like(part_ref)
    part_ref[0:rows, :] = total.astype(BF16)


def experts_kernel(
    outer,
    part_ref,
    tokens_ref,
    gain_ref,
    routes_ref,
    route_weights_ref,
    gate_hbm,
    up_hbm,
    down_hbm,
    out_ref,
    gate,
    up,
    down,
    part_in,
    residual,
    xbuf,
    core_out,
    core_in,
    core_own,
    plane,
    plane_in,
    back_out,
    back_in,
    w_sem,
    t_sem,
    z_send,
    a_send,
    c_send,
    x_recv,
    core_sem,
    plane_send,
    plane_recv,
    back_send,
    back_recv,
):
    rows, width = tokens_ref.shape
    pad = part_ref.shape[0]
    cols = out_ref.shape[1]
    me, t = lax.axis_index("ep"), lax.axis_index("tp")
    o, a, c = me // SLICES, (me // 2) % 2, me % 2
    na, nc, nt = 1 - a, 1 - c, 1 - t

    def device(o_, a_, c_, t_):
        return (o_ * SLICES + a_ * 2 + c_, t_)

    def send(src, dst, s_sem, r_sem, target):
        copy = pltpu.make_async_remote_copy(
            src_ref=src,
            dst_ref=dst,
            send_sem=s_sem,
            recv_sem=r_sem,
            device_id=target,
            device_id_type=MESH,
        )
        copy.start()
        sent.append(copy)
        return copy

    sent = []
    w_copies = [
        pltpu.make_async_copy(src.at[0], dst, w_sem.at[i])
        for i, (src, dst) in enumerate(((gate_hbm, gate), (up_hbm, up), (down_hbm, down)))
    ]
    barrier = pltpu.get_barrier_semaphore()
    others = [lax.rem(o + i, outer) for i in range(1, outer)]
    peers = [device(o_, a, c, t) for o_ in others]
    peers += [device(o, na, c, t), device(o, a, nc, t), device(o, a, c, nt), device(o, na, c, nt)]
    for peer in peers:
        pl.semaphore_signal(barrier, inc=1, device_id=peer, device_id_type=MESH)
    for copy in w_copies:
        copy.start()
    pl.semaphore_wait(barrier, len(peers))

    swap = send(part_ref, part_in, t_sem.at[0], t_sem.at[1], device(o, a, c, nt))
    swap.wait_recv()
    token_f = tokens_ref[...].astype(F32)
    mixed = part_ref[0:rows, :].astype(F32) + part_in[0:rows, :].astype(F32)
    mixed = mixed.astype(BF16).astype(F32)
    summed = (token_f + mixed).astype(BF16).astype(F32)
    for i in range(width // cols):
        residual[i, 0:rows, :] = summed[:, i * cols : (i + 1) * cols]
    ffn_in = (summed * inverse_rms(summed) * gain_ref[...]).astype(BF16)
    xbuf[c, a, o] = jnp.zeros((pad, width), BF16)
    xbuf[c, a, o, 0:rows, :] = ffn_in

    mine = xbuf.at[c, a, o]
    for i, o_ in enumerate(others):
        send(mine, mine, z_send.at[i], x_recv.at[c, a, o], device(o_, a, c, t))
    order = [o] + others
    for i, o_ in enumerate(order):
        block, sem = xbuf.at[c, a, o_], x_recv.at[c, a, o_]
        if i:
            pltpu.make_async_copy(block, block, sem).wait()
        send(block, block, a_send.at[i], sem, device(o, na, c, t))
        send(block, block, c_send.at[0, i], sem, device(o, a, nc, t))
    for i, o_ in enumerate(order):
        block, sem = xbuf.at[c, na, o_], x_recv.at[c, na, o_]
        pltpu.make_async_copy(block, block, sem).wait()
        send(block, block, c_send.at[1, i], sem, device(o, a, nc, t))
    for copy in w_copies:
        copy.wait()

    def experts(half):
        x = half.reshape(2 * outer * pad, width)
        g = dot(x, gate[...])
        hidden = (g / (1.0 + jnp.exp(-g)) * dot(x, up[...])).astype(BF16)
        return dot(hidden, down[...]).reshape(2, outer, pad, width)

    for a_ in (a, na):
        for o_ in order:
            block, sem = xbuf.at[nc, a_, o_], x_recv.at[nc, a_, o_]
            pltpu.make_async_copy(block, block, sem).wait()
    core_out[...] = experts(xbuf[nc]).astype(BF16)
    swap = send(core_out, core_in, core_sem.at[0], core_sem.at[1], device(o, a, nc, t))
    core_own[...] = experts(xbuf[c])
    swap.wait_recv()
    for i in range(width // cols):
        at = slice(i * cols, (i + 1) * cols)
        plane[:, i] = (core_own[:, :, :, at] + core_in[:, :, :, at].astype(F32)).astype(BF16)
    hops = [
        send(
            plane.at[a_, t_],
            plane_in.at[i],
            plane_send.at[i],
            plane_recv.at[i],
            device(o, a_, c, t_),
        )
        for i, (a_, t_) in enumerate(((na, nt), (na, t), (a, nt)))
    ]
    total = plane[a, t].astype(F32)
    for i in (1, 2, 0):
        hops[i].wait_recv()
        total = total + plane_in[i].astype(F32)
    back_out[...] = total.astype(BF16)
    for i, o_ in enumerate(others):
        send(
            back_out.at[o_], back_in.at[o], back_send.at[i], back_recv.at[o], device(o_, a, c, t)
        )
    back_in[o] = back_out[o]
    for o_ in others:
        block = back_in.at[o_]
        pltpu.make_async_copy(block, block, back_recv.at[o_]).wait()
    result = residual[t, 0:rows, :]
    routes = routes_ref[...]
    route_weights = route_weights_ref[...]
    for e in range(outer):
        weight = jnp.sum(jnp.where(routes == e, route_weights, 0.0), axis=1, keepdims=True)
        result = result + weight * back_in[e, 0:rows, :].astype(F32)
    out_ref[...] = result.astype(BF16)
    for copy in sent:
        copy.wait_send()


def body(
    tokens,
    attn_gain,
    query_weight,
    key_weight,
    value_weight,
    forget_weight,
    forget_bias,
    out_weight,
    key_cache,
    value_cache,
    cum_forget,
    lengths,
    ffn_gain,
    routes,
    route_weights,
    gate_weight,
    up_weight,
    down_weight,
):
    tp_count = lax.axis_size("tp")
    outer = lax.axis_size("ep") // SLICES
    rows, width = tokens.shape
    cols = width // tp_count
    pad = (rows + 15) // 16 * 16
    kv_local, hd, span = key_cache.shape[1:]
    heads = cum_forget.shape[1]
    lanes = kv_local * hd
    units = gate_weight.shape[2]
    hbm, vmem, smem = (
        pl.BlockSpec(memory_space=space) for space in (pltpu.HBM, pltpu.VMEM, pltpu.SMEM)
    )
    dma = pltpu.SemaphoreType.DMA
    part = pl.pallas_call(
        attention_kernel,
        out_shape=jax.ShapeDtypeStruct((pad, width), BF16),
        in_specs=[vmem, vmem, smem, smem, hbm, hbm, hbm, vmem, hbm, hbm, hbm, hbm],
        out_specs=vmem,
        scratch_shapes=[
            pltpu.VMEM(query_weight.shape, BF16),
            pltpu.VMEM(key_weight.shape, BF16),
            pltpu.VMEM(value_weight.shape, BF16),
            pltpu.VMEM(out_weight.shape, BF16),
            pltpu.VMEM(key_cache.shape, BF16),
            pltpu.VMEM(value_cache.shape, BF16),
            pltpu.VMEM(cum_forget.shape, F32),
            pltpu.VMEM((pad * 8, lanes), F32),
            pltpu.VMEM((pad * 8, lanes), F32),
            pltpu.VMEM((pad * 8, lanes), F32),
            dma((4,)),
            dma((rows,)),
            dma((rows,)),
            dma((rows,)),
        ],
        compiler_params=pltpu.CompilerParams(vmem_limit_bytes=24 * 2**20),
        name="attention",
    )(
        tokens,
        attn_gain.reshape(1, width),
        forget_bias,
        lengths,
        query_weight,
        key_weight,
        value_weight,
        forget_weight.T,
        out_weight,
        key_cache,
        value_cache,
        cum_forget,
    )
    return pl.pallas_call(
        functools.partial(experts_kernel, outer),
        out_shape=jax.ShapeDtypeStruct((rows, cols), BF16),
        in_specs=[vmem] * 5 + [hbm] * 3,
        out_specs=vmem,
        scratch_shapes=[
            pltpu.VMEM(gate_weight.shape[1:], BF16),
            pltpu.VMEM(up_weight.shape[1:], BF16),
            pltpu.VMEM(down_weight.shape[1:], BF16),
            pltpu.VMEM((pad, width), BF16),
            pltpu.VMEM((tp_count, pad, cols), F32),
            pltpu.VMEM((2, 2, outer, pad, width), BF16),
            pltpu.VMEM((2, outer, pad, width), BF16),
            pltpu.VMEM((2, outer, pad, width), BF16),
            pltpu.VMEM((2, outer, pad, width), F32),
            pltpu.VMEM((2, tp_count, outer, pad, cols), BF16),
            pltpu.VMEM((3, outer, pad, cols), BF16),
            pltpu.VMEM((outer, pad, cols), BF16),
            pltpu.VMEM((outer, pad, cols), BF16),
            dma((3,)),
            dma((2,)),
            dma((outer - 1,)),
            dma((outer,)),
            dma((2, outer)),
            dma((2, 2, outer)),
            dma((2,)),
            dma((3,)),
            dma((3,)),
            dma((outer - 1,)),
            dma((outer,)),
        ],
        compiler_params=pltpu.CompilerParams(
            collective_id=0, has_side_effects=True, vmem_limit_bytes=48 * 2**20
        ),
        name="experts",
    )(
        part,
        tokens,
        ffn_gain.reshape(1, width),
        routes,
        route_weights,
        gate_weight,
        up_weight,
        down_weight,
    )


def solution(mesh):
    return jax.shard_map(
        body,
        mesh=mesh,
        in_specs=(
            P("ep", None),
            P(),
            P(None, "tp"),
            P(None, "tp"),
            P(None, "tp"),
            P(None, "tp"),
            P("tp"),
            P("tp", None),
            P("ep", "tp", None, None),
            P("ep", "tp", None, None),
            P("ep", "tp", None),
            P("ep"),
            P(),
            P("ep", None),
            P("ep", None),
            P("ep", None, "tp"),
            P("ep", None, "tp"),
            P("ep", "tp", None),
        ),
        out_specs=P("ep", "tp"),
        check_vma=False,
    )
```

```python
import functools

import jax
import jax.numpy as jnp
from jax import lax
from jax.experimental import pallas as pl
from jax.experimental.pallas import tpu as pltpu
from jax.sharding import PartitionSpec as P

HEADS = 8
KVH = 4
HD = 64
SLICES = 4
EPSILON = 1e-06
GROUP_SEQS = 4
MESH = pl.DeviceIdType.MESH
F32 = jnp.float32
BF16 = jnp.bfloat16


def inverse_rms(values):
    return lax.rsqrt(jnp.sum(values * values, axis=-1, keepdims=True) / values.shape[-1] + EPSILON)


def dot(a, b):
    return jnp.dot(a, b, preferred_element_type=F32)


def dot_nt(a, b):
    return lax.dot_general(a, b, (((1,), (1,)), ((), ())), preferred_element_type=F32)


def layer_kernel(
    outer,
    tokens_hbm,
    attn_gain_hbm,
    bias_hbm,
    lengths_hbm,
    wq_hbm,
    wk_hbm,
    wv_hbm,
    wf_hbm,
    wo_hbm,
    keys_hbm,
    values_hbm,
    cum_hbm,
    ffn_gain_hbm,
    routes_hbm,
    route_weights_hbm,
    gate_hbm,
    up_hbm,
    down_hbm,
    out_ref,
    tokens_ref,
    attn_gain_ref,
    bias_ref,
    lengths_ref,
    wq,
    wk,
    wv,
    wf_ref,
    wo,
    keys,
    values,
    cum,
    ffn_gain_ref,
    routes_ref,
    route_weights_ref,
    gate,
    up,
    down,
    q_rows,
    own_rows,
    out_rows,
    part,
    part_in,
    residual,
    xbuf,
    core_out,
    core_in,
    core_own,
    plane,
    plane_in,
    back_out,
    back_in,
    w_sem,
    k_sem,
    v_sem,
    c_sem,
    t_sem,
    z_send,
    a_send,
    c_send,
    x_recv,
    core_send,
    core_recv,
    plane_send,
    plane_recv,
    back_send,
    back_recv,
):
    rows, width = tokens_ref.shape
    pad = part.shape[0]
    cols = out_ref.shape[1]
    kv_local, hd, span = keys.shape[1:]
    heads = cum.shape[1]
    group = heads // kv_local
    lanes = kv_local * hd
    scale = hd ** (-0.5)
    me, t = lax.axis_index("ep"), lax.axis_index("tp")
    o, a, c = me // SLICES, (me // 2) % 2, me % 2
    na, nc, nt = 1 - a, 1 - c, 1 - t

    def local(i, src, dst):
        copy = pltpu.make_async_copy(src, dst, w_sem.at[i])
        copy.start()
        return copy

    first_copies = [
        local(i, src, dst)
        for i, (src, dst) in enumerate(
            (
                (tokens_hbm, tokens_ref),
                (attn_gain_hbm, attn_gain_ref),
                (bias_hbm, bias_ref),
                (lengths_hbm, lengths_ref),
                (wf_hbm, wf_ref),
                (wq_hbm, wq),
                (wk_hbm, wk),
                (wv_hbm, wv),
            )
        )
    ]

    def device(o_, a_, c_, t_):
        return (o_ * SLICES + a_ * 2 + c_, t_)

    near = sorted(range(1, outer), key=lambda i: min(i, outer - i))
    others = [lax.rem(o + i, outer) for i in near]
    barrier = pltpu.get_barrier_semaphore()
    peers = [device(o_, a, c, t) for o_ in others]
    peers += [device(o, na, c, t), device(o, a, nc, t), device(o, a, c, nt), device(o, na, c, nt)]
    for peer in peers:
        pl.semaphore_signal(barrier, inc=1, device_id=peer, device_id_type=MESH)

    copies = []
    for b in range(rows):
        trio = (
            pltpu.make_async_copy(keys_hbm.at[b], keys.at[b], k_sem.at[b]),
            pltpu.make_async_copy(cum_hbm.at[b], cum.at[b], c_sem.at[b]),
            pltpu.make_async_copy(values_hbm.at[b], values.at[b], v_sem.at[b]),
        )
        for copy in trio:
            copy.start()
        copies.append(trio)
    wo_copy = local(8, wo_hbm, wo)
    late_copies = [
        local(i + 9, src, dst)
        for i, (src, dst) in enumerate(
            (
                (ffn_gain_hbm, ffn_gain_ref),
                (routes_hbm, routes_ref),
                (route_weights_hbm, route_weights_ref),
                (gate_hbm.at[0], gate),
                (up_hbm.at[0], up),
                (down_hbm.at[0], down),
            )
        )
    ]

    for copy in first_copies:
        copy.wait()
    token_f = tokens_ref[...].astype(F32)
    normed = (token_f * inverse_rms(token_f) * attn_gain_ref[...]).astype(BF16)
    head_id = lax.broadcasted_iota(jnp.int32, (heads, 1), 0)
    bias = jnp.zeros((heads, 1), F32)
    for h in range(heads):
        bias = jnp.where(head_id == h, bias_ref[h], bias)
    log_forget = jax.nn.log_sigmoid(dot_nt(wf_ref[...], normed) + bias)
    queries = dot(normed, wq[...]).astype(BF16).astype(F32)
    new_keys = dot(normed, wk[...]).astype(BF16).astype(F32)
    new_values = dot(normed, wv[...]).astype(BF16).astype(F32)
    lane_kv = lax.broadcasted_iota(jnp.int32, (rows, lanes), 1) // hd
    q_rows[...] = jnp.zeros_like(q_rows)
    own_rows[...] = jnp.zeros_like(own_rows)
    for h in range(heads):
        kv = h // group
        base = (h * hd) // lanes * lanes
        segment = queries[:, base : base + lanes]
        shift = (kv * hd - (h * hd - base)) % lanes
        if shift:
            segment = pltpu.roll(segment, shift, 1)
        segment = jnp.where(lane_kv == kv, segment, 0.0)
        q_rows[pl.ds(h, rows, stride=8), :] = segment
        own_rows[pl.ds(h, rows, stride=8), :] = segment * new_keys

    position = lax.broadcasted_iota(jnp.int32, (heads, span), 1)
    for first in range(0, rows, GROUP_SEQS):
        members = range(first, min(first + GROUP_SEQS, rows))
        for b in members:
            for copy in copies[b]:
                copy.wait()
        scores = [
            dot(q_rows[b * 8 : b * 8 + 8, :].astype(BF16), keys[b].reshape(lanes, span))[:heads]
            for b in members
        ]
        weights, own = [], []
        for b, score in zip(members, scores):
            cumul = cum[b]
            length = lengths_ref[b]
            last = jnp.sum(jnp.where(position == length - 1, cumul, 0.0), axis=1, keepdims=True)
            score = score * scale + (last - cumul) + log_forget[:, b : b + 1]
            score = jnp.where(position < length, score, -jnp.inf)
            self_score = (
                jnp.sum(own_rows[b * 8 : b * 8 + 8, :], axis=1, keepdims=True)[:heads] * scale
            )
            top = jnp.maximum(jnp.max(score, axis=1, keepdims=True), self_score)
            expo = jnp.exp(score - top)
            own_exp = jnp.exp(self_score - top)
            inverse = 1.0 / (jnp.sum(expo, axis=1, keepdims=True) + own_exp)
            weights.append((expo * inverse).astype(BF16))
            own.append((own_exp * inverse).astype(BF16).astype(F32))
        for b, weight, own_weight in zip(members, weights, own):
            mixed = dot_nt(weight, values[b].reshape(lanes, span))
            out_rows[b * 8 : b * 8 + heads, :] = mixed + own_weight * new_values[b : b + 1, :]

    blocks = []
    for h in range(heads):
        kv = h // group
        base = (h * hd) // lanes * lanes
        segment = out_rows[pl.ds(h, rows, stride=8), :]
        segment = jnp.where(lane_kv == kv, segment, 0.0)
        shift = (h * hd - base - kv * hd) % lanes
        if shift:
            segment = pltpu.roll(segment, shift, 1)
        if base // lanes == len(blocks):
            blocks.append(segment)
        else:
            blocks[-1] = blocks[-1] + segment
    wo_copy.wait()
    total = None
    for i, block in enumerate(blocks):
        term = dot(block.astype(BF16), wo[i * lanes : (i + 1) * lanes, :])
        total = term if total is None else total + term
    part[...] = jnp.zeros_like(part)
    part[0:rows, :] = total.astype(BF16)

    sent = []

    def send(src, dst, s_sem, r_sem, target):
        copy = pltpu.make_async_remote_copy(
            src_ref=src,
            dst_ref=dst,
            send_sem=s_sem,
            recv_sem=r_sem,
            device_id=target,
            device_id_type=MESH,
        )
        copy.start()
        sent.append(copy)
        return copy

    pl.semaphore_wait(barrier, len(peers))
    swap = send(part, part_in, t_sem.at[0], t_sem.at[1], device(o, a, c, nt))
    for copy in late_copies:
        copy.wait()
    expert = lax.broadcasted_iota(jnp.int32, (outer, rows), 0)
    row_weights = jnp.zeros((outer, rows), F32)
    for k in range(routes_ref.shape[0]):
        named = routes_ref[k : k + 1, :] == expert
        row_weights = row_weights + jnp.where(named, route_weights_ref[k : k + 1, :], 0.0)
    swap.wait_recv()
    mixed = part[0:rows, :].astype(F32) + part_in[0:rows, :].astype(F32)
    mixed = mixed.astype(BF16).astype(F32)
    summed = (token_f + mixed).astype(BF16).astype(F32)
    for i in range(width // cols):
        residual[i, 0:rows, :] = summed[:, i * cols : (i + 1) * cols]
    ffn_in = (summed * inverse_rms(summed) * ffn_gain_ref[...]).astype(BF16)
    xbuf[c, a, o] = jnp.zeros((pad, width), BF16)
    xbuf[c, a, o, 0:rows, :] = ffn_in

    mine = xbuf.at[c, a, o]
    order = [o] + others
    for i in reversed(range(len(others))):
        send(mine, mine, z_send.at[i], x_recv.at[c, a, o], device(others[i], a, c, t))
    for i, o_ in enumerate(order):
        block, sem = xbuf.at[c, a, o_], x_recv.at[c, a, o_]
        if i:
            pltpu.make_async_copy(block, block, sem).wait()
        send(block, block, a_send.at[i], sem, device(o, na, c, t))
        send(block, block, c_send.at[0, i], sem, device(o, a, nc, t))
    for i, o_ in enumerate(order):
        block, sem = xbuf.at[c, na, o_], x_recv.at[c, na, o_]
        pltpu.make_async_copy(block, block, sem).wait()
        send(block, block, c_send.at[1, i], sem, device(o, a, nc, t))

    def experts(half):
        x = half.reshape(2 * outer * pad, width)
        g = dot(x, gate[...])
        hidden = (g / (1.0 + jnp.exp(-g)) * dot(x, up[...])).astype(BF16)
        return dot(hidden, down[...]).reshape(2, outer, pad, width)

    for a_ in (a, na):
        for o_ in order:
            block, sem = xbuf.at[nc, a_, o_], x_recv.at[nc, a_, o_]
            pltpu.make_async_copy(block, block, sem).wait()
    order = others[::-1] + [o]
    core_out[...] = experts(xbuf[nc]).astype(BF16)
    for o_ in order:
        send(
            core_out.at[:, o_],
            core_in.at[:, o_],
            core_send.at[o_],
            core_recv.at[o_],
            device(o, a, nc, t),
        )
    core_own[...] = experts(xbuf[c])
    targets = ((na, nt), (na, t), (a, nt))
    for o_ in order:
        block = core_in.at[:, o_]
        pltpu.make_async_copy(block, block, core_recv.at[o_]).wait()
        both = core_own[:, o_] + core_in[:, o_].astype(F32)
        for i in range(width // cols):
            plane[:, i, o_] = both[:, :, i * cols : (i + 1) * cols].astype(BF16)
        for i, (a_, t_) in enumerate(targets):
            send(
                plane.at[a_, t_, o_],
                plane_in.at[i, o_],
                plane_send.at[i, o_],
                plane_recv.at[i, o_],
                device(o, a_, c, t_),
            )
    for n, o_ in enumerate(order):
        total = plane[a, t, o_].astype(F32)
        for i in range(len(targets)):
            block = plane_in.at[i, o_]
            pltpu.make_async_copy(block, block, plane_recv.at[i, o_]).wait()
            total = total + plane_in[i, o_].astype(F32)
        if n < len(others):
            back_out[n] = total.astype(BF16)
            send(
                back_out.at[n], back_in.at[o], back_send.at[n], back_recv.at[o], device(o_, a, c, t)
            )
        else:
            back_in[o] = total.astype(BF16)
    for o_ in others:
        block = back_in.at[o_]
        pltpu.make_async_copy(block, block, back_recv.at[o_]).wait()
    result = residual[t, 0:rows, :]
    square = (rows, rows)
    diagonal = lax.broadcasted_iota(jnp.int32, square, 0) == lax.broadcasted_iota(
        jnp.int32, square, 1
    )
    for e in range(outer):
        weight = jnp.sum(
            jnp.where(diagonal, row_weights[e : e + 1, :], 0.0), axis=1, keepdims=True
        )
        result = result + weight * back_in[e, 0:rows, :].astype(F32)
    out_ref[...] = result.astype(BF16)
    for copy in sent:
        copy.wait_send()


def body(
    tokens,
    attn_gain,
    query_weight,
    key_weight,
    value_weight,
    forget_weight,
    forget_bias,
    out_weight,
    key_cache,
    value_cache,
    cum_forget,
    lengths,
    ffn_gain,
    routes,
    route_weights,
    gate_weight,
    up_weight,
    down_weight,
):
    tp_count = lax.axis_size("tp")
    outer = lax.axis_size("ep") // SLICES
    rows, width = tokens.shape
    cols = width // tp_count
    pad = (rows + 15) // 16 * 16
    kv_local, hd = key_cache.shape[1:3]
    lanes = kv_local * hd
    dma = pltpu.SemaphoreType.DMA
    operands = (
        tokens,
        attn_gain.reshape(1, width),
        forget_bias,
        lengths,
        query_weight,
        key_weight,
        value_weight,
        forget_weight.T,
        out_weight,
        key_cache,
        value_cache,
        cum_forget,
        ffn_gain.reshape(1, width),
        routes.T,
        route_weights.T,
        gate_weight,
        up_weight,
        down_weight,
    )
    held = []
    for i, operand in enumerate(operands):
        space = pltpu.SMEM if i in (2, 3) else pltpu.VMEM
        held.append(space(operand.shape[1:] if i >= 15 else operand.shape, operand.dtype))
    return pl.pallas_call(
        functools.partial(layer_kernel, outer),
        out_shape=jax.ShapeDtypeStruct((rows, cols), BF16),
        in_specs=[pl.BlockSpec(memory_space=pltpu.HBM)] * len(operands),
        out_specs=pl.BlockSpec(memory_space=pltpu.VMEM),
        scratch_shapes=held
        + [
            pltpu.VMEM((pad * 8, lanes), F32),
            pltpu.VMEM((pad * 8, lanes), F32),
            pltpu.VMEM((pad * 8, lanes), F32),
            pltpu.VMEM((pad, width), BF16),
            pltpu.VMEM((pad, width), BF16),
            pltpu.VMEM((tp_count, pad, cols), F32),
            pltpu.VMEM((2, 2, outer, pad, width), BF16),
            pltpu.VMEM((2, outer, pad, width), BF16),
            pltpu.VMEM((2, outer, pad, width), BF16),
            pltpu.VMEM((2, outer, pad, width), F32),
            pltpu.VMEM((2, tp_count, outer, pad, cols), BF16),
            pltpu.VMEM((3, outer, pad, cols), BF16),
            pltpu.VMEM((outer - 1, pad, cols), BF16),
            pltpu.VMEM((outer, pad, cols), BF16),
            dma((15,)),
            dma((rows,)),
            dma((rows,)),
            dma((rows,)),
            dma((2,)),
            dma((outer - 1,)),
            dma((outer,)),
            dma((2, outer)),
            dma((2, 2, outer)),
            dma((outer,)),
            dma((outer,)),
            dma((3, outer)),
            dma((3, outer)),
            dma((outer - 1,)),
            dma((outer,)),
        ],
        compiler_params=pltpu.CompilerParams(
            collective_id=0, has_side_effects=True, vmem_limit_bytes=60 * 2**20
        ),
        name="layer",
    )(*operands)


def solution(mesh):
    return jax.shard_map(
        body,
        mesh=mesh,
        in_specs=(
            P("ep", None),
            P(),
            P(None, "tp"),
            P(None, "tp"),
            P(None, "tp"),
            P(None, "tp"),
            P("tp"),
            P("tp", None),
            P("ep", "tp", None, None),
            P("ep", "tp", None, None),
            P("ep", "tp", None),
            P("ep"),
            P(),
            P("ep", None),
            P("ep", None),
            P("ep", None, "tp"),
            P("ep", None, "tp"),
            P("ep", "tp", None),
        ),
        out_specs=P("ep", "tp"),
        check_vma=False,
    )
```

```python
import functools

import jax
import jax.numpy as jnp
from jax import lax
from jax.experimental import pallas as pl
from jax.experimental.pallas import tpu as pltpu
from jax.sharding import PartitionSpec as P

HEADS = 8
KVH = 4
HD = 64
SLICES = 4
EPSILON = 1e-06
GROUP_SEQS = 4
PACK = 2
MESH = pl.DeviceIdType.MESH
F32 = jnp.float32
BF16 = jnp.bfloat16


def inverse_rms(values):
    return lax.rsqrt(jnp.sum(values * values, axis=-1, keepdims=True) / values.shape[-1] + EPSILON)


def dot(a, b):
    return jnp.dot(a, b, preferred_element_type=F32)


def dot_nt(a, b):
    return lax.dot_general(a, b, (((1,), (1,)), ((), ())), preferred_element_type=F32)


def layer_kernel(
    outer,
    tokens_hbm,
    attn_gain_hbm,
    bias_hbm,
    lengths_hbm,
    wq_hbm,
    wk_hbm,
    wv_hbm,
    wf_hbm,
    wo_hbm,
    keys_hbm,
    values_hbm,
    cum_hbm,
    ffn_gain_hbm,
    routes_hbm,
    route_weights_hbm,
    gate_hbm,
    up_hbm,
    down_hbm,
    out_ref,
    tokens_ref,
    attn_gain_ref,
    bias_ref,
    lengths_ref,
    wq,
    wk,
    wv,
    wf_ref,
    wo,
    keys,
    values,
    cum,
    ffn_gain_ref,
    routes_ref,
    route_weights_ref,
    gate,
    up,
    down,
    q_rows,
    own_rows,
    out_rows,
    part,
    part_in,
    residual,
    xbuf,
    core_out,
    core_in,
    core_own,
    plane,
    plane_in,
    back_out,
    back_in,
    w_sem,
    k_sem,
    v_sem,
    c_sem,
    t_sem,
    z_send,
    a_send,
    c_send,
    x_recv,
    core_send,
    core_recv,
    plane_send,
    plane_recv,
    back_send,
    back_recv,
):
    rows, width = tokens_ref.shape
    pad = part.shape[0]
    cols = out_ref.shape[1]
    kv_local, hd, span = keys.shape[1:]
    heads = cum.shape[1]
    group = heads // kv_local
    lanes = kv_local * hd
    scale = hd ** (-0.5)
    me, t = lax.axis_index("ep"), lax.axis_index("tp")
    o, a, c = me // SLICES, (me // 2) % 2, me % 2
    na, nc, nt = 1 - a, 1 - c, 1 - t

    def local(i, src, dst):
        copy = pltpu.make_async_copy(src, dst, w_sem.at[i])
        copy.start()
        return copy

    first_copies = [
        local(i, src, dst)
        for i, (src, dst) in enumerate(
            (
                (tokens_hbm, tokens_ref),
                (attn_gain_hbm, attn_gain_ref),
                (bias_hbm, bias_ref),
                (lengths_hbm, lengths_ref),
                (wf_hbm, wf_ref),
                (wq_hbm, wq),
                (wk_hbm, wk),
                (wv_hbm, wv),
            )
        )
    ]

    def device(o_, a_, c_, t_):
        return (o_ * SLICES + a_ * 2 + c_, t_)

    near = sorted(range(1, outer), key=lambda i: min(i, outer - i))
    others = [lax.rem(o + i, outer) for i in near]
    barrier = pltpu.get_barrier_semaphore()
    peers = [device(o_, a, c, t) for o_ in others]
    peers += [device(o, na, c, t), device(o, a, nc, t), device(o, a, c, nt), device(o, na, c, nt)]
    for peer in peers:
        pl.semaphore_signal(barrier, inc=1, device_id=peer, device_id_type=MESH)

    copies = []
    for b in range(rows):
        trio = (
            pltpu.make_async_copy(keys_hbm.at[b], keys.at[b], k_sem.at[b]),
            pltpu.make_async_copy(cum_hbm.at[b], cum.at[b], c_sem.at[b]),
            pltpu.make_async_copy(values_hbm.at[b], values.at[b], v_sem.at[b]),
        )
        for copy in trio:
            copy.start()
        copies.append(trio)
    wo_copy = local(8, wo_hbm, wo)
    late_copies = [
        local(i + 9, src, dst)
        for i, (src, dst) in enumerate(
            (
                (ffn_gain_hbm, ffn_gain_ref),
                (routes_hbm, routes_ref),
                (route_weights_hbm, route_weights_ref),
                (gate_hbm.at[0], gate),
                (up_hbm.at[0], up),
                (down_hbm.at[0], down),
            )
        )
    ]

    for copy in first_copies:
        copy.wait()
    token_f = tokens_ref[...].astype(F32)
    normed = (token_f * inverse_rms(token_f) * attn_gain_ref[...]).astype(BF16)
    head_id = lax.broadcasted_iota(jnp.int32, (heads, 1), 0)
    bias = jnp.zeros((heads, 1), F32)
    for h in range(heads):
        bias = jnp.where(head_id == h, bias_ref[h], bias)
    log_forget = jax.nn.log_sigmoid(dot_nt(wf_ref[...], normed) + bias)
    queries = dot(normed, wq[...]).astype(BF16).astype(F32)
    new_keys = dot(normed, wk[...]).astype(BF16).astype(F32)
    new_values = dot(normed, wv[...]).astype(BF16).astype(F32)
    lane_kv = lax.broadcasted_iota(jnp.int32, (rows, lanes), 1) // hd
    q_rows[...] = jnp.zeros_like(q_rows)
    own_rows[...] = jnp.zeros_like(own_rows)
    for h in range(heads):
        kv = h // group
        base = (h * hd) // lanes * lanes
        segment = queries[:, base : base + lanes]
        shift = (kv * hd - (h * hd - base)) % lanes
        if shift:
            segment = pltpu.roll(segment, shift, 1)
        segment = jnp.where(lane_kv == kv, segment, 0.0)
        q_rows[pl.ds(h, rows, stride=heads), :] = segment
        own_rows[pl.ds(h, rows, stride=heads), :] = segment * new_keys

    def stacked(pieces):
        return pieces[0] if len(pieces) == 1 else jnp.concatenate(pieces, axis=0)

    for first in range(0, rows, GROUP_SEQS):
        final = min(first + GROUP_SEQS, rows)
        packs = [range(b, min(b + PACK, final)) for b in range(first, final, PACK)]
        scores, weights, own = [], [], []
        for pack in packs:
            for b in pack:
                copies[b][0].wait()
                copies[b][1].wait()
            n = len(pack)
            tile = q_rows[pack[0] * heads : (pack[0] + n) * heads, :]
            member = lax.broadcasted_iota(jnp.int32, tile.shape, 0) // heads
            parts = [jnp.where(member == i, tile, 0.0) for i in range(n)]
            tile = parts[0] if n == 1 else jnp.concatenate(parts, axis=1)
            block = keys[pack[0] : pack[0] + n].reshape(n * lanes, span)
            scores.append(dot(tile.astype(BF16), block))
        for pack, score in zip(packs, scores):
            n = len(pack)
            at = slice(pack[0] * heads, (pack[0] + n) * heads)
            member = lax.broadcasted_iota(jnp.int32, (n * heads, 1), 0) // heads
            length = jnp.zeros((n * heads, 1), jnp.int32)
            for i, b in enumerate(pack):
                length = jnp.where(member == i, lengths_ref[b], length)
            cumul = stacked([cum[b] for b in pack])
            forget = stacked([log_forget[:, b : b + 1] for b in pack])
            position = lax.broadcasted_iota(jnp.int32, (n * heads, span), 1)
            last = jnp.sum(jnp.where(position == length - 1, cumul, 0.0), axis=1, keepdims=True)
            score = jnp.where(position < length, score * scale - cumul, -jnp.inf)
            self_score = jnp.sum(own_rows[at, :], axis=1, keepdims=True) * scale
            self_score = self_score - (last + forget)
            top = jnp.maximum(jnp.max(score, axis=1, keepdims=True), self_score)
            expo = jnp.exp(score - top)
            own_exp = jnp.exp(self_score - top)
            inverse = 1.0 / (jnp.sum(expo, axis=1, keepdims=True) + own_exp)
            weights.append((expo * inverse).astype(BF16))
            own.append((own_exp * inverse).astype(BF16).astype(F32))
        for b in range(first, final):
            copies[b][2].wait()
        for pack, weight, own_weight in zip(packs, weights, own):
            n = len(pack)
            mixed = dot_nt(weight, values[pack[0] : pack[0] + n].reshape(n * lanes, span))
            member = lax.broadcasted_iota(jnp.int32, (n * heads, lanes), 0) // heads
            value, fresh = mixed[:, :lanes], new_values[pack[0] : pack[0] + 1, :]
            for i in range(1, n):
                value = jnp.where(member == i, mixed[:, i * lanes : (i + 1) * lanes], value)
                fresh = jnp.where(member == i, new_values[pack[i] : pack[i] + 1, :], fresh)
            out_rows[pack[0] * heads : (pack[0] + n) * heads, :] = value + own_weight * fresh

    blocks = []
    for h in range(heads):
        kv = h // group
        base = (h * hd) // lanes * lanes
        segment = out_rows[pl.ds(h, rows, stride=heads), :]
        segment = jnp.where(lane_kv == kv, segment, 0.0)
        shift = (h * hd - base - kv * hd) % lanes
        if shift:
            segment = pltpu.roll(segment, shift, 1)
        if base // lanes == len(blocks):
            blocks.append(segment)
        else:
            blocks[-1] = blocks[-1] + segment
    wo_copy.wait()
    total = None
    for i, block in enumerate(blocks):
        term = dot(block.astype(BF16), wo[i * lanes : (i + 1) * lanes, :])
        total = term if total is None else total + term
    part[...] = jnp.zeros_like(part)
    part[0:rows, :] = total.astype(BF16)

    sent = []

    def send(src, dst, s_sem, r_sem, target):
        copy = pltpu.make_async_remote_copy(
            src_ref=src,
            dst_ref=dst,
            send_sem=s_sem,
            recv_sem=r_sem,
            device_id=target,
            device_id_type=MESH,
        )
        copy.start()
        sent.append(copy)
        return copy

    pl.semaphore_wait(barrier, len(peers))
    swap = send(part, part_in, t_sem.at[0], t_sem.at[1], device(o, a, c, nt))
    for copy in late_copies:
        copy.wait()
    expert = lax.broadcasted_iota(jnp.int32, (outer, rows), 0)
    row_weights = jnp.zeros((outer, rows), F32)
    for k in range(routes_ref.shape[0]):
        named = routes_ref[k : k + 1, :] == expert
        row_weights = row_weights + jnp.where(named, route_weights_ref[k : k + 1, :], 0.0)
    swap.wait_recv()
    mixed = part[0:rows, :].astype(F32) + part_in[0:rows, :].astype(F32)
    mixed = mixed.astype(BF16).astype(F32)
    summed = (token_f + mixed).astype(BF16).astype(F32)
    for i in range(width // cols):
        residual[i, 0:rows, :] = summed[:, i * cols : (i + 1) * cols]
    ffn_in = (summed * inverse_rms(summed) * ffn_gain_ref[...]).astype(BF16)
    xbuf[c, a, o] = jnp.zeros((pad, width), BF16)
    xbuf[c, a, o, 0:rows, :] = ffn_in

    mine = xbuf.at[c, a, o]
    order = [o] + others
    for i in reversed(range(len(others))):
        send(mine, mine, z_send.at[i], x_recv.at[c, a, o], device(others[i], a, c, t))
    for i, o_ in enumerate(order):
        block, sem = xbuf.at[c, a, o_], x_recv.at[c, a, o_]
        if i:
            pltpu.make_async_copy(block, block, sem).wait()
        send(block, block, a_send.at[i], sem, device(o, na, c, t))
        send(block, block, c_send.at[0, i], sem, device(o, a, nc, t))
    for i, o_ in enumerate(order):
        block, sem = xbuf.at[c, na, o_], x_recv.at[c, na, o_]
        pltpu.make_async_copy(block, block, sem).wait()
        send(block, block, c_send.at[1, i], sem, device(o, a, nc, t))

    def experts(half):
        x = half.reshape(2 * outer * pad, width)
        g = dot(x, gate[...])
        hidden = (g / (1.0 + jnp.exp(-g)) * dot(x, up[...])).astype(BF16)
        return dot(hidden, down[...]).reshape(2, outer, pad, width)

    for a_ in (a, na):
        for o_ in order:
            block, sem = xbuf.at[nc, a_, o_], x_recv.at[nc, a_, o_]
            pltpu.make_async_copy(block, block, sem).wait()
    order = others[::-1] + [o]
    core_out[...] = experts(xbuf[nc]).astype(BF16)
    for o_ in order:
        send(
            core_out.at[:, o_],
            core_in.at[:, o_],
            core_send.at[o_],
            core_recv.at[o_],
            device(o, a, nc, t),
        )
    core_own[...] = experts(xbuf[c])
    targets = ((na, nt), (na, t), (a, nt))
    for o_ in order:
        block = core_in.at[:, o_]
        pltpu.make_async_copy(block, block, core_recv.at[o_]).wait()
        both = core_own[:, o_] + core_in[:, o_].astype(F32)
        for i in range(width // cols):
            plane[:, i, o_] = both[:, :, i * cols : (i + 1) * cols].astype(BF16)
        for i, (a_, t_) in enumerate(targets):
            send(
                plane.at[a_, t_, o_],
                plane_in.at[i, o_],
                plane_send.at[i, o_],
                plane_recv.at[i, o_],
                device(o, a_, c, t_),
            )
    for n, o_ in enumerate(order):
        total = plane[a, t, o_].astype(F32)
        for i in range(len(targets)):
            block = plane_in.at[i, o_]
            pltpu.make_async_copy(block, block, plane_recv.at[i, o_]).wait()
            total = total + plane_in[i, o_].astype(F32)
        if n < len(others):
            back_out[n] = total.astype(BF16)
            send(
                back_out.at[n], back_in.at[o], back_send.at[n], back_recv.at[o], device(o_, a, c, t)
            )
        else:
            back_in[o] = total.astype(BF16)
    for o_ in others:
        block = back_in.at[o_]
        pltpu.make_async_copy(block, block, back_recv.at[o_]).wait()
    result = residual[t, 0:rows, :]
    square = (rows, rows)
    diagonal = lax.broadcasted_iota(jnp.int32, square, 0) == lax.broadcasted_iota(
        jnp.int32, square, 1
    )
    for e in range(outer):
        weight = jnp.sum(
            jnp.where(diagonal, row_weights[e : e + 1, :], 0.0), axis=1, keepdims=True
        )
        result = result + weight * back_in[e, 0:rows, :].astype(F32)
    out_ref[...] = result.astype(BF16)
    for copy in sent:
        copy.wait_send()


def body(
    tokens,
    attn_gain,
    query_weight,
    key_weight,
    value_weight,
    forget_weight,
    forget_bias,
    out_weight,
    key_cache,
    value_cache,
    cum_forget,
    lengths,
    ffn_gain,
    routes,
    route_weights,
    gate_weight,
    up_weight,
    down_weight,
):
    tp_count = lax.axis_size("tp")
    outer = lax.axis_size("ep") // SLICES
    rows, width = tokens.shape
    cols = width // tp_count
    pad = (rows + 15) // 16 * 16
    kv_local, hd = key_cache.shape[1:3]
    heads = cum_forget.shape[1]
    lanes = kv_local * hd
    dma = pltpu.SemaphoreType.DMA
    operands = (
        tokens,
        attn_gain.reshape(1, width),
        forget_bias,
        lengths,
        query_weight,
        key_weight,
        value_weight,
        forget_weight.T,
        out_weight,
        key_cache,
        value_cache,
        cum_forget,
        ffn_gain.reshape(1, width),
        routes.T,
        route_weights.T,
        gate_weight,
        up_weight,
        down_weight,
    )
    held = []
    for i, operand in enumerate(operands):
        space = pltpu.SMEM if i in (2, 3) else pltpu.VMEM
        held.append(space(operand.shape[1:] if i >= 15 else operand.shape, operand.dtype))
    return pl.pallas_call(
        functools.partial(layer_kernel, outer),
        out_shape=jax.ShapeDtypeStruct((rows, cols), BF16),
        in_specs=[pl.BlockSpec(memory_space=pltpu.HBM)] * len(operands),
        out_specs=pl.BlockSpec(memory_space=pltpu.VMEM),
        scratch_shapes=held
        + [
            pltpu.VMEM((pad * heads, lanes), F32),
            pltpu.VMEM((pad * heads, lanes), F32),
            pltpu.VMEM((pad * heads, lanes), F32),
            pltpu.VMEM((pad, width), BF16),
            pltpu.VMEM((pad, width), BF16),
            pltpu.VMEM((tp_count, pad, cols), F32),
            pltpu.VMEM((2, 2, outer, pad, width), BF16),
            pltpu.VMEM((2, outer, pad, width), BF16),
            pltpu.VMEM((2, outer, pad, width), BF16),
            pltpu.VMEM((2, outer, pad, width), F32),
            pltpu.VMEM((2, tp_count, outer, pad, cols), BF16),
            pltpu.VMEM((3, outer, pad, cols), BF16),
            pltpu.VMEM((outer - 1, pad, cols), BF16),
            pltpu.VMEM((outer, pad, cols), BF16),
            dma((15,)),
            dma((rows,)),
            dma((rows,)),
            dma((rows,)),
            dma((2,)),
            dma((outer - 1,)),
            dma((outer,)),
            dma((2, outer)),
            dma((2, 2, outer)),
            dma((outer,)),
            dma((outer,)),
            dma((3, outer)),
            dma((3, outer)),
            dma((outer - 1,)),
            dma((outer,)),
        ],
        compiler_params=pltpu.CompilerParams(
            collective_id=0, has_side_effects=True, vmem_limit_bytes=60 * 2**20
        ),
        name="layer",
    )(*operands)


def solution(mesh):
    return jax.shard_map(
        body,
        mesh=mesh,
        in_specs=(
            P("ep", None),
            P(),
            P(None, "tp"),
            P(None, "tp"),
            P(None, "tp"),
            P(None, "tp"),
            P("tp"),
            P("tp", None),
            P("ep", "tp", None, None),
            P("ep", "tp", None, None),
            P("ep", "tp", None),
            P("ep"),
            P(),
            P("ep", None),
            P("ep", None),
            P("ep", None, "tp"),
            P("ep", None, "tp"),
            P("ep", "tp", None),
        ),
        out_specs=P("ep", "tp"),
        check_vma=False,
    )
```
